32 devices in a mesh: sp: 8 (over z, y), tp: 4 (over x, core).
Axes of the slice: x: 2, y: 2, z: 4, core: 2. Of those that a mesh axis runs over, the one named last changes fastest.
Arguments:
- residual_in: bfloat16 [3072, 2048], P(('sp', 'tp')), may hold values from -6 to 6
- queries: bfloat16 [3072, 2048], P('sp', 'tp'), may hold values from -180 to 180
- keys: bfloat16 [3072, 2048], P('sp', 'tp'), may hold values from -9 to 9
- values: bfloat16 [3072, 2048], P('sp', 'tp'), may hold values from -6 to 6
- mix_lambda: float32 [16], P('tp'), may hold values from 0.3 to 0.8
- head_gain: float32 [128], replicated, may hold values from 0.1 to 1.9
- out_weight: bfloat16 [2048, 2048], P('tp'), may hold values from -0.125 to 0.125
- norm_gain: float32 [2048], replicated, may hold values from 0.1 to 1.9
- gate_weight: bfloat16 [2048, 5632], P('sp', 'tp'), may hold values from -0.125 to 0.125
- up_weight: bfloat16 [2048, 5632], P('sp', 'tp'), may hold values from -0.125 to 0.125
- down_weight: bfloat16 [5632, 2048], P('tp', 'sp'), may hold values from -0.078125 to 0.078125
Outputs:
- layer_out: bfloat16 [3072, 2048], P(('sp', 'tp'))
The draws below stay inside these ranges and needn't reach their ends.
All inputs are finite; a program needn't handle non-finite values.
Results may differ from the reference program's by a relative error of at most 0.014.
Values may be sent and summed in bfloat16 or wider, within the bound.
A program may use at most 128 MiB of HBM per device.

```python
import math
import jax
import jax.numpy as jnp
from jax import lax

D = 2048
H = 16
DH = 64
VD = 128
FF = 5632
TOKENS = 3072


def shared_keys(key):
    base = jax.random.fold_in(key, 101)
    drawn = jnp.clip(1.3 * jax.random.normal(jax.random.fold_in(base, 1), (TOKENS, H * 2 * DH), jnp.float32), -8.0, 8.0)
    return drawn


def draw_keys(key, part):
    drawn = shared_keys(key)
    return drawn.astype(jnp.bfloat16)


def draw_queries(key, part):
    base = jax.random.fold_in(key, 202)
    drawn = jnp.clip(1.3 * jax.random.normal(jax.random.fold_in(base, 1), (TOKENS, H * 2 * DH), jnp.float32), -8.0, 8.0)
    return drawn.astype(jnp.bfloat16)


def block_levels(own_key, dims, shards, low, largest):
    loudness, own = 1.0, jax.random.fold_in(own_key, 6)
    for position, parts in shards:
        heights = jnp.exp(jax.random.uniform(jax.random.fold_in(own, position), (parts,), jnp.float32, low / len(shards), largest / len(shards)))
        loudness = loudness * jnp.repeat(heights, dims[position] // parts).reshape([-1 if axis == position else 1 for axis in range(len(dims))])
    return loudness


def bell_draw(key, extent, width, limit, cuts=(), kind=jnp.bfloat16):
    values = jax.random.normal(key, extent, jnp.float32) * width
    if len(cuts) > 0:
        values = block_levels(key, extent, cuts, -0.22, 0.18) * values
    return jnp.clip(values, min=-limit, max=limit).astype(kind)


def setup_inputs(seed: int = 0) -> dict:
    arg_keys = jax.random.split(jax.random.key(seed), 12)
    return {
        "residual_in": bell_draw(arg_keys[0], (TOKENS, D), 1.0, 6.0, ((0, 32),)),
        "queries": draw_queries(jax.random.fold_in(arg_keys[11], 71), 0),
        "keys": draw_keys(jax.random.fold_in(arg_keys[11], 71), 0),
        "values": bell_draw(arg_keys[3], (TOKENS, H * VD), 1.0, 6.0, ((0, 8), (1, 4))),
        "mix_lambda": jnp.clip(0.3 + 0.5 * jax.random.uniform(arg_keys[4], (H,), jnp.float32) ** block_levels(arg_keys[4], (H,), ((0, 4),), -0.2, 0.2), 0.3, 0.8),
        "head_gain": jnp.clip(1.0 + 0.18 * jax.random.normal(arg_keys[5], (VD,), jnp.float32), 0.1, 1.9),
        "out_weight": bell_draw(arg_keys[6], (H * VD, D), (H * VD) ** -0.5, 0.125, ((0, 4),)),
        "norm_gain": jnp.clip(1.0 + 0.18 * jax.random.normal(arg_keys[7], (D,), jnp.float32), 0.1, 1.9),
        "gate_weight": bell_draw(arg_keys[8], (D, FF), D ** -0.5, 0.125, ((0, 8), (1, 4))),
        "up_weight": bell_draw(arg_keys[9], (D, FF), D ** -0.5, 0.125, ((0, 8), (1, 4))),
        "down_weight": bell_draw(arg_keys[10], (FF, D), FF ** -0.5, 0.078125, ((0, 4), (1, 8))),
    }


def head_rows(args):
    query_head, key_head, value_head, weight_two, head_gain = args
    block_rows = math.gcd(512, TOKENS)
    blocks = query_head.reshape(TOKENS // block_rows, block_rows, 2, DH)
    key_float = key_head.astype(jnp.float32)
    value_float = value_head.astype(jnp.float32)

    def one_block(query_block):
        scores = jnp.einsum('qcd,kcd->cqk', query_block.astype(jnp.float32), key_float) / math.sqrt(DH)
        top = lax.optimization_barrier(jnp.max(scores, axis=-1, keepdims=True))
        expo = jnp.exp(scores - top)
        total = lax.optimization_barrier(jnp.sum(expo, axis=-1, keepdims=True))
        probs = lax.optimization_barrier(expo.astype(jnp.bfloat16)).astype(jnp.float32)
        maps = jnp.einsum('cqk,ke->cqe', probs, value_float) / total
        mixed = maps[0] - weight_two * maps[1]
        scale = lax.rsqrt(lax.optimization_barrier(jnp.mean(mixed * mixed, axis=-1, keepdims=True)) + 1e-06)
        return (mixed * scale * head_gain).astype(jnp.bfloat16)
    return lax.map(one_block, blocks).reshape(TOKENS, VD)

def reference(residual_in, queries, keys, values, mix_lambda, head_gain, out_weight, norm_gain, gate_weight, up_weight, down_weight):
    query_heads = jnp.transpose(queries.reshape(TOKENS, H, 2, DH), (1, 0, 2, 3))
    key_heads = jnp.transpose(keys.reshape(TOKENS, H, 2, DH), (1, 0, 2, 3))
    value_heads = jnp.transpose(values.reshape(TOKENS, H, VD), (1, 0, 2))
    gains = jnp.broadcast_to(head_gain, (H, VD))
    per_head = lax.map(head_rows, (query_heads, key_heads, value_heads, mix_lambda, gains))
    attended = jnp.transpose(per_head, (1, 0, 2)).reshape(TOKENS, H * VD)
    after_mix = residual_in.astype(jnp.float32) + jnp.dot(attended, out_weight, preferred_element_type=jnp.float32)
    scale = lax.rsqrt(lax.optimization_barrier(jnp.mean(after_mix * after_mix, axis=-1, keepdims=True)) + 1e-06)
    normed = (after_mix * scale * norm_gain).astype(jnp.bfloat16)
    gate = jnp.dot(normed, gate_weight, preferred_element_type=jnp.float32)
    up = jnp.dot(normed, up_weight, preferred_element_type=jnp.float32)
    hidden = (jax.nn.silu(gate) * up).astype(jnp.bfloat16)
    mixer = jnp.dot(hidden, down_weight, preferred_element_type=jnp.float32)
    return (after_mix + 0.5 * mixer).astype(jnp.bfloat16)
```

```python
import functools
import math

import jax
import jax.numpy as jnp
from jax import lax
from jax.experimental import pallas as pl
from jax.experimental.pallas import tpu as pltpu
from jax.sharding import Mesh, PartitionSpec as P

DH = 64
VD = 128
LOG2E = 1.4426950408889634

MESH = pl.DeviceIdType.MESH
AXES = ("za", "yb", "xb", "cb")


def remote(src, dst, send, recv, **where):
    return pltpu.make_async_remote_copy(
        src_ref=src, dst_ref=dst, send_sem=send, recv_sem=recv, device_id=where, device_id_type=MESH
    )


def near_first(z, k, nz):
    m = jnp.minimum(z, nz - 1 - z)
    near = z + ((k + 1) // 2 if k % 2 else -(k // 2))
    far = jnp.where(z < nz - 1 - z, k, nz - 1 - k)
    return jnp.where(k <= 2 * m, near, far)


def layer_kernel(n, lam_ref, gain_ref, ngain_ref, res_hbm, q_hbm, k_hbm, v_hbm, ow_hbm, gate_hbm, up_hbm, down_hbm,
                 out, wp,
                 qs, kk, vx, osend, att, ow, res, w, stage, om, oc_send, oc_recv, ox_send, ox_recv,
                 got, mine, c_send, c_recv, z_send, z_recv,
                 in_s, st_s, qz_s, qz_r, ky_s, ky_r, wl_s, wz_s, wz_r, wx_s, wx_r, wy_s, wy_r,
                 wxy_s, wxy_r, wyx_s, wyx_r, o_s, o_r, oc_s, oc_r, ox_s, ox_r,
                 az_s, az_r, ac_s, ac_r, rc_s, rc_r, rz_s, rz_r):
    nz, ny, nx, nc, heads, aligned = n
    z, y, x, c = (lax.axis_index(name) for name in AXES)
    other = nc - 1 - c
    tok, own = qs.shape[1:]
    rows, model = res.shape
    pair = nc * rows
    hid, depth = gate_hbm.shape[0] // nz, gate_hbm.shape[1]
    cut = hid // 16 * 8

    barrier = pltpu.get_barrier_semaphore()
    for d in range(1, nz):
        pl.semaphore_signal(barrier, inc=1, device_id={"za": lax.rem(z + d, nz)}, device_id_type=MESH)
    for f in range(1, ny):
        pl.semaphore_signal(barrier, inc=1, device_id={"yb": lax.rem(y + f, ny)}, device_id_type=MESH)
    for e in range(1, nx):
        pl.semaphore_signal(barrier, inc=1, device_id={"xb": lax.rem(x + e, nx)}, device_id_type=MESH)
    for e in range(1, nc):
        pl.semaphore_signal(barrier, inc=1, device_id={"cb": other}, device_id_type=MESH)
    pl.semaphore_wait(barrier, nz + ny + nx + nc - 4)

    def tokens(zz, yy):
        return pl.ds(pl.multiple_of((zz * ny + yy) * tok, tok), tok)

    def kv_parts(zz, yy):
        at = tokens(zz, yy)
        return [kk.at[at]] + [vx.at[at, 2 * h * VD : (2 * h + 1) * VD] for h in range(heads)]

    def kv_sources(zp):
        base = zp * own
        return [k_hbm.at[:, pl.ds(pl.multiple_of(base, 128), own)]] + [
            v_hbm.at[:, pl.ds(pl.multiple_of(base + h * VD, 128), VD)] for h in range(heads)
        ]

    def q_source(zp):
        return q_hbm.at[:, pl.ds(pl.multiple_of(zp * own, 128), own)]

    nkv = 1 + heads

    def qkv_copies(d):
        zp = lax.rem(z + d, nz)
        pairs = list(zip(kv_sources(zp), kv_parts(z, y))) + [(q_source(zp), qs.at[z])]
        return [remote(s, t, qz_s.at[i, d], qz_r.at[i, z], za=zp) for i, (s, t) in enumerate(pairs)]

    def qkv_take(zp):
        pairs = list(zip(kv_sources(z), kv_parts(zp, y))) + [(q_source(z), qs.at[zp])]
        return [remote(s, t, qz_s.at[i, 0], qz_r.at[i, zp], za=zp) for i, (s, t) in enumerate(pairs)]

    def kv_pass(d, f):
        zp, yp = lax.rem(z + d, nz), lax.rem(y + f, ny)
        to = kv_parts(zp, y)
        fro = to if d else kv_sources(z)
        return [remote(s, t, ky_s.at[i, d, f], ky_r.at[i, zp, y], yb=yp) for i, (s, t) in enumerate(zip(fro, to))]

    def kv_take(zp, yp):
        to = kv_parts(zp, yp)
        return [remote(t, t, ky_s.at[i, 0, 0], ky_r.at[i, zp, yp], yb=yp) for i, t in enumerate(to)]

    mats = (gate_hbm, up_hbm, down_hbm)

    def place(m, xx, zz, yy, start=0, size=hid):
        at = zz * ny + yy
        r = pl.ds(pl.multiple_of(xx * hid + start, 8), size)
        if aligned:
            return w.at[m, r, pl.ds(pl.multiple_of(at * depth, depth), depth)]
        return wp.at[at, m, r]

    every = slice(None)

    def w_copies(d):
        zp = lax.rem(z + d, nz)
        return [
            remote(a.at[pl.ds(pl.multiple_of(zp * hid, 8), hid)], place(m, x, z, y), wz_s.at[m, d], wz_r.at[m, z], za=zp)
            for m, a in enumerate(mats)
        ]

    def w_local():
        return [
            pltpu.make_async_copy(a.at[pl.ds(pl.multiple_of(z * hid, 8), hid)], place(m, x, z, y), wl_s.at[m])
            for m, a in enumerate(mats)
        ]

    def w_x(d, e):
        zp, xp = lax.rem(z + d, nz), lax.rem(x + e, nx)
        at = place(every, x, zp, y)
        return remote(at, at, wx_s.at[d, e], wx_r.at[zp, x], xb=xp)

    def w_y(d, f):
        zp, yp = lax.rem(z + d, nz), lax.rem(y + f, ny)
        at = place(every, x, zp, y)
        return remote(at, at, wy_s.at[d, f], wy_r.at[zp, y], yb=yp)

    def w_xy(d, e, f):
        zp, xp, yp = lax.rem(z + d, nz), lax.rem(x + e, nx), lax.rem(y + f, ny)
        at = place(every, xp, zp, y, 0, cut)
        return remote(at, at, wxy_s.at[d, e, f], wxy_r.at[zp, xp, y], yb=yp)

    def w_yx(d, f, e):
        zp, xp, yp = lax.rem(z + d, nz), lax.rem(x + e, nx), lax.rem(y + f, ny)
        at = place(every, x, zp, yp, cut, hid - cut)
        return remote(at, at, wyx_s.at[d, f, e], wyx_r.at[zp, yp, x], xb=xp)

    def w_spread(d):
        for e in range(1, nx):
            w_x(d, e).start()
        for f in range(1, ny):
            w_y(d, f).start()

    def w_take(d):
        zp = lax.rem(z + d, nz)
        for m, a in enumerate(mats):
            remote(a.at[pl.ds(0, hid)], place(m, x, zp, y), wz_s.at[m, 0], wz_r.at[m, zp], za=zp).wait_recv()
        w_spread(d)

    def w_turn(d):
        zp = lax.rem(z + d, nz)
        for e in range(1, nx):
            xp = lax.rem(x + e, nx)
            at = place(every, xp, zp, y)
            remote(at, at, wx_s.at[d, e], wx_r.at[zp, xp], xb=xp).wait_recv()
            for f in range(1, ny):
                w_xy(d, e, f).start()
        for f in range(1, ny):
            yp = lax.rem(y + f, ny)
            at = place(every, x, zp, yp)
            remote(at, at, wy_s.at[d, f], wy_r.at[zp, yp], yb=yp).wait_recv()
            for e in range(1, nx):
                w_yx(d, f, e).start()

    def w_done():
        for d in range(nz):
            zp = lax.rem(z + d, nz)
            for e in range(1, nx):
                xp = lax.rem(x + e, nx)
                for f in range(1, ny):
                    yp = lax.rem(y + f, ny)
                    at = place(every, xp, zp, yp, 0, cut)
                    remote(at, at, wxy_s.at[d, e, f], wxy_r.at[zp, xp, yp], yb=yp).wait_recv()
                    at = place(every, xp, zp, yp, cut, hid - cut)
                    remote(at, at, wyx_s.at[d, f, e], wyx_r.at[zp, yp, xp], xb=xp).wait_recv()
        if not aligned:
            for at in range(nz * ny):
                copy = pltpu.make_async_copy(wp.at[at], stage, st_s)
                copy.start()
                copy.wait()
                for m in range(3):
                    w[m, :, at * depth : (at + 1) * depth] = stage[m]

    for d in range(nz - 1, 0, -1):
        for copy in qkv_copies(d):
            copy.start()
    for f in range(1, ny):
        for copy in kv_pass(0, f):
            copy.start()
    locals_in = [
        pltpu.make_async_copy(s, t, in_s.at[i])
        for i, (s, t) in enumerate(
            list(zip(kv_sources(z), kv_parts(z, y))) + [(q_source(z), qs.at[z]), (ow_hbm, ow), (res_hbm, res)]
        )
    ]
    for copy in locals_in:
        copy.start()
    for copy in w_local():
        copy.start()
    for d in range(nz - 1, 1, -1):
        for copy in w_copies(d):
            copy.start()
    for h in range(heads):
        vx[:, (2 * h + 1) * VD : (2 * h + 2) * VD] = jnp.ones((vx.shape[0], VD), jnp.bfloat16)
    for copy in w_local():
        copy.wait()
    w_spread(0)
    for copy in locals_in:
        copy.wait()
    for d in range(1, nz):
        zp = lax.rem(z + d, nz)
        for copy in qkv_take(zp):
            copy.wait_recv()
        for f in range(1, ny):
            for copy in kv_pass(d, f):
                copy.start()
    for d in range(nz):
        zp = lax.rem(z + d, nz)
        for f in range(1, ny):
            for copy in kv_take(zp, lax.rem(y + f, ny)):
                copy.wait_recv()
    w_turn(0)

    scale = LOG2E / math.sqrt(DH)
    block_rows = osend.shape[1]
    per = tok // block_rows

    def o_copy(i):
        zq = lax.rem(z + 1 + i // per, nz)
        off = pl.multiple_of(lax.rem(i, per) * block_rows, block_rows)
        to = att.at[pl.ds(off, block_rows), pl.ds(pl.multiple_of(z * own, 128), own)]
        return remote(osend.at[i], to, o_s.at[i], o_r.at[z, lax.rem(i, per)], za=zq)

    def block(i, carry):
        zq = lax.rem(z + 1 + i // per, nz)
        off = pl.multiple_of(lax.rem(i, per) * block_rows, block_rows)
        for h in range(heads):
            cols = slice(h * VD, (h + 1) * VD)
            q = qs[zq, pl.ds(off, block_rows), cols]
            lane = lax.broadcasted_iota(jnp.int32, q.shape, 1)
            maps = []
            for half in range(2):
                qc = jnp.where((lane >= DH) if half else (lane < DH), q, jnp.zeros_like(q))
                s = lax.dot_general(
                    qc, kk[:, cols], (((1,), (1,)), ((), ())), preferred_element_type=jnp.float32
                )
                top = jnp.max(s, axis=-1, keepdims=True)
                e = jnp.exp2((s - top) * scale).astype(jnp.bfloat16)
                o = jnp.dot(
                    e, vx[:, 2 * h * VD : (2 * h + 2) * VD], preferred_element_type=jnp.float32
                )
                maps.append(o[:, :VD] / o[:, VD:])
            mixed = maps[0] - lam_ref[z * heads + h] * maps[1]
            norm = lax.rsqrt(jnp.mean(mixed * mixed, axis=-1, keepdims=True) + 1e-06)
            osend[i, :, cols] = (mixed * norm * gain_ref[...]).astype(jnp.bfloat16)

        @pl.when(zq != z)
        def _():
            o_copy(i).start()

        if nz > 1:
            @pl.when(i == nz * per // 2)
            def _():
                w_take(1)

        return carry

    lax.fori_loop(0, nz * per, block, 0)
    if nz > 2:
        for copy in w_copies(1):
            copy.start()
    elif nz == 2:
        pass
    for j in range(per):
        att[j * block_rows : (j + 1) * block_rows, pl.ds(pl.multiple_of(z * own, 128), own)] = osend[(nz - 1) * per + j]
    if nz > 1:
        w_turn(1)
    for d in range(2, nz - 1):
        w_take(d)
    for d in range(1, nz):
        zp = lax.rem(z + d, nz)
        for j in range(per):
            to = att.at[pl.ds(j * block_rows, block_rows), pl.ds(pl.multiple_of(zp * own, 128), own)]
            remote(osend.at[j], to, o_s.at[j], o_r.at[zp, j], za=zp).wait_recv()

    def split(part):
        if nc == 1:
            return part, None
        low, high = part[:rows], part[rows:]
        return jnp.where(c == 0, low, high), jnp.where(c == 0, high, low)

    def oc_copy(e):
        return remote(oc_send.at[e], oc_recv.at[e], oc_s.at[e], oc_r.at[e], cb=other)

    def ox_copy(e):
        return remote(ox_send.at[e], ox_recv.at[e], ox_s.at[e], ox_r.at[e], xb=lax.rem(x + e, nx))

    ring = list(range(1, nx)) + [0]
    for e in ring:
        xp = lax.rem(x + e, nx)
        part = jnp.dot(
            att[pl.ds(pl.multiple_of(xp * pair, 8), pair)], ow[...], preferred_element_type=jnp.float32
        )
        keep, send = split(part)
        om[e] = keep
        if nc > 1:
            oc_send[e] = send.astype(jnp.bfloat16)
            oc_copy(e).start()
    for e in ring:
        total = om[e]
        if nc > 1:
            oc_copy(e).wait_recv()
            total = total + oc_recv[e].astype(jnp.float32)
        if e:
            ox_send[e] = total.astype(jnp.bfloat16)
            ox_copy(e).start()
    for d in range(2, nz - 1):
        w_turn(d)
    after = res[...].astype(jnp.float32) + total
    for e in range(1, nx):
        ox_copy(e).wait_recv()
        after = after + ox_recv[e].astype(jnp.float32)
    om[0] = after
    row_scale = lax.rsqrt(jnp.mean(after * after, axis=-1, keepdims=True) + 1e-06)

    def slot(zp, cc):
        return got.at[zp, pl.ds(pl.multiple_of(cc * rows, 8), rows)]

    def ag_z(zp, to):
        return remote(slot(zp, c), slot(zp, c), az_s.at[zp, jnp.where(to > z, 1, 0)], az_r.at[zp], za=to)

    def ag_c(zp):
        return remote(slot(zp, c), slot(zp, c), ac_s.at[zp], ac_r.at[zp], cb=other)

    def rs_c(zp):
        return remote(c_send.at[zp], c_recv.at[zp], rc_s.at[zp], rc_r.at[zp], cb=other)

    def rs_z(zp):
        return remote(z_send.at[zp], z_recv.at[z], rz_s.at[zp], rz_r.at[z], za=zp)

    got[z, pl.ds(pl.multiple_of(c * rows, 8), rows)] = (after * row_scale * ngain_ref[...]).astype(jnp.bfloat16)

    def onward(zp, act):
        to = jnp.where(zp < z, z + 1, z - 1)

        @pl.when(jnp.logical_and(to >= 0, to < nz))
        def _():
            act(ag_z(zp, to))

    def own_ways(act):
        @pl.when(z + 1 < nz)
        def _():
            act(ag_z(z, z + 1))

        @pl.when(z > 0)
        def _():
            act(ag_z(z, z - 1))

    own_ways(lambda copy: copy.start())
    if nc > 1:
        ag_c(z).start()

    def pass_on(k):
        zp = near_first(z, k, nz)
        ag_z(zp, jnp.where(zp < z, z - 1, z + 1)).wait_recv()
        onward(zp, lambda copy: copy.start())
        if nc > 1:
            ag_c(zp).start()

    contract = (((1,), (1,)), ((), ()))

    def compute(k):
        zp = near_first(z, k, nz)
        if nc > 1:
            remote(slot(zp, other), slot(zp, other), ac_s.at[zp], ac_r.at[zp], cb=other).wait_recv()
        tokens_in = got[zp]
        gate = lax.dot_general(tokens_in, w[0], contract, preferred_element_type=jnp.float32)
        up = lax.dot_general(tokens_in, w[1], contract, preferred_element_type=jnp.float32)
        hidden = (jax.nn.silu(gate) * up).astype(jnp.bfloat16)
        keep, send = split(jnp.dot(hidden, w[2], preferred_element_type=jnp.float32))
        mine[zp] = keep
        if nc > 1:
            c_send[zp] = send.astype(jnp.bfloat16)
            rs_c(zp).start()

    def finish(k):
        zp = near_first(z, k, nz)
        total = mine[zp]
        if nc > 1:
            rs_c(zp).wait_recv()
            total = total + c_recv[zp].astype(jnp.float32)
        if k:
            z_send[zp] = total.astype(jnp.bfloat16)
            rs_z(zp).start()
        return total

    if nz > 1:
        if nz > 2:
            w_take(nz - 1)
        pass_on(1)
        if nz > 2:
            w_turn(nz - 1)
    for k in range(2, nz - 1):
        pass_on(k)
    w_done()
    order = list(range(1, nz)) + [0]
    for i, k in enumerate(order):
        if k == nz - 1 and nz > 2:
            pass_on(k)
        compute(k)
        if i:
            finish(order[i - 1])
    total = finish(0)
    for k in range(1, nz):
        zp = near_first(z, k, nz)
        remote(z_send.at[zp], z_recv.at[zp], rz_s.at[zp], rz_r.at[zp], za=zp).wait_recv()
        total = total + z_recv[zp].astype(jnp.float32)
    out[...] = (om[0] + 0.5 * total).astype(jnp.bfloat16)

    for d in range(1, nz):
        for copy in qkv_copies(d) + w_copies(d):
            copy.wait_send()
    for d in range(nz):
        for f in range(1, ny):
            for copy in kv_pass(d, f):
                copy.wait_send()
            w_y(d, f).wait_send()
        for e in range(1, nx):
            w_x(d, e).wait_send()
            for f in range(1, ny):
                w_xy(d, e, f).wait_send()
                w_yx(d, f, e).wait_send()
    for i in range((nz - 1) * per):
        o_copy(i).wait_send()
    for e in range(nx):
        if nc > 1:
            oc_copy(e).wait_send()
        if e:
            ox_copy(e).wait_send()
    own_ways(lambda copy: copy.wait_send())
    for k in range(nz):
        zp = near_first(z, k, nz)
        if k:
            onward(zp, lambda copy: copy.wait_send())
            rs_z(zp).wait_send()
        if nc > 1:
            ag_c(zp).wait_send()
            rs_c(zp).wait_send()


def body(
    residual_in,
    queries,
    keys,
    values,
    mix_lambda,
    head_gain,
    out_weight,
    norm_gain,
    gate_weight,
    up_weight,
    down_weight,
):
    nz, ny, nx, nc = (lax.axis_size(name) for name in AXES)
    tok, width = queries.shape
    rows, model = residual_in.shape
    heads = mix_lambda.shape[0] // nz
    own = width // nz
    depth = down_weight.shape[1]
    hid = down_weight.shape[0] // nz
    aligned = depth % 128 == 0
    nsp = nz * ny
    block_rows = 2 * rows
    per = tok // block_rows
    vmem = pl.BlockSpec(memory_space=pltpu.VMEM)
    smem = pl.BlockSpec(memory_space=pltpu.SMEM)
    hbm = pl.BlockSpec(memory_space=pl.ANY)
    dma = pltpu.SemaphoreType.DMA
    bf16, f32 = jnp.bfloat16, jnp.float32
    parts = (8, 128) if aligned else (3, nx * hid, depth)
    return pl.pallas_call(
        functools.partial(layer_kernel, (nz, ny, nx, nc, heads, aligned)),
        out_shape=(
            jax.ShapeDtypeStruct((rows, model), bf16),
            jax.ShapeDtypeStruct(parts if aligned else (nsp, *parts), bf16),
        ),
        in_specs=[smem, vmem, vmem] + [hbm] * 8,
        out_specs=(vmem, hbm),
        scratch_shapes=[
            pltpu.VMEM((nz, tok, own), bf16),
            pltpu.VMEM((nsp * tok, own), bf16),
            pltpu.VMEM((nsp * tok, 2 * own), bf16),
            pltpu.VMEM((nz * per, block_rows, own), bf16),
            pltpu.VMEM((tok, width), bf16),
            pltpu.VMEM((width, model), bf16),
            pltpu.VMEM((rows, model), bf16),
            pltpu.VMEM((3, nx * hid, model), bf16),
            pltpu.VMEM(parts, bf16),
            pltpu.VMEM((nx, rows, model), f32),
            pltpu.VMEM((nx, rows, model), bf16),
            pltpu.VMEM((nx, rows, model), bf16),
            pltpu.VMEM((nx, rows, model), bf16),
            pltpu.VMEM((nx, rows, model), bf16),
            pltpu.VMEM((nz, nc * rows, model), bf16),
            pltpu.VMEM((nz, rows, model), f32),
            pltpu.VMEM((nz, rows, model), bf16),
            pltpu.VMEM((nz, rows, model), bf16),
            pltpu.VMEM((nz, rows, model), bf16),
            pltpu.VMEM((nz, rows, model), bf16),
            dma((heads + 4,)), dma,
            dma((heads + 2, nz)), dma((heads + 2, nz)),
            dma((heads + 1, nz, ny)), dma((heads + 1, nz, ny)),
            dma((3,)),
            dma((3, nz)), dma((3, nz)),
            dma((nz, nx)), dma((nz, nx)),
            dma((nz, ny)), dma((nz, ny)),
            dma((nz, nx, ny)), dma((nz, nx, ny)),
            dma((nz, ny, nx)), dma((nz, ny, nx)),
            dma((nz * per,)), dma((nz, per)),
            dma((nx,)), dma((nx,)),
            dma((nx,)), dma((nx,)),
            dma((nz, 2)), dma((nz,)),
            dma((nz,)), dma((nz,)),
            dma((nz,)), dma((nz,)),
            dma((nz,)), dma((nz,)),
        ],
        compiler_params=pltpu.CompilerParams(
            collective_id=1, has_side_effects=True, vmem_limit_bytes=62 * 1024 * 1024
        ),
    )(
        mix_lambda,
        head_gain.reshape(1, VD),
        norm_gain.reshape(1, model),
        residual_in,
        queries,
        keys,
        values,
        out_weight,
        gate_weight.T,
        up_weight.T,
        down_weight,
    )[0]


def solution(mesh):
    sp, tp = mesh.shape["sp"], mesh.shape["tp"]

    def run(*args):
        heads_local = args[4].shape[0] // tp
        za = math.gcd(heads_local, sp)
        nc = math.gcd(tp, 2)
        cut = Mesh(mesh.devices.reshape(za, sp // za, tp // nc, nc), AXES)
        s, t = ("za", "yb"), ("xb", "cb")
        return jax.shard_map(
            body,
            mesh=cut,
            in_specs=(
                P(AXES, None),
                P(s, t),
                P(s, t),
                P(s, t),
                P(t),
                P(),
                P(t, None),
                P(),
                P(s, t),
                P(s, t),
                P(t, s),
            ),
            out_specs=P(AXES, None),
            check_vma=False,
        )(*args)

    return run
```

```python
import functools
import math

import jax
import jax.numpy as jnp
from jax import lax
from jax.experimental import pallas as pl
from jax.experimental.pallas import tpu as pltpu
from jax.sharding import Mesh, PartitionSpec as P

DH = 64
VD = 128
LOG2E = 1.4426950408889634

MESH = pl.DeviceIdType.MESH
AXES = ("za", "yb", "xb", "cb")


def remote(src, dst, send, recv, **where):
    return pltpu.make_async_remote_copy(
        src_ref=src, dst_ref=dst, send_sem=send, recv_sem=recv, device_id=where, device_id_type=MESH
    )


def across_first(z, k, nz):
    half = max(nz // 2, 1)
    if k < nz - half:
        return jnp.where(z < half, half + k, half - 1 - k)
    return z // half * half + lax.rem(z + 1 + k - (nz - half), half)


def layer_kernel(n, lam_ref, gain_ref, ngain_ref, res_hbm, q_hbm, k_hbm, v_hbm, ow_hbm, gate_hbm, up_hbm, down_hbm,
                 out, wp,
                 qs, kk, vx, osend, att, ow, res, w, stage, om, oc_send, oc_recv, ox_send, ox_recv,
                 got, mine, c_send, c_recv, z_send, z_recv, t_recv,
                 in_s, st_s, qz_s, qz_r, ky_s, ky_r, wl_s, wz_s, wz_r, wx_s, wx_r, wy_s, wy_r,
                 wxy_s, wxy_r, wyx_s, wyx_r, o_s, o_r, oc_s, oc_r, ox_s, ox_r,
                 az_s, az_r, ac_s, ac_r, rc_s, rc_r, rz_s, rz_r, rt_r):
    nz, ny, nx, nc, heads, aligned = n
    z, y, x, c = (lax.axis_index(name) for name in AXES)
    other = nc - 1 - c
    tok, own = qs.shape[1:]
    rows, model = res.shape
    pair = nc * rows
    hid, depth = gate_hbm.shape[0] // nz, gate_hbm.shape[1]
    cut = hid // 16 * 8

    barrier = pltpu.get_barrier_semaphore()
    for d in range(1, nz):
        pl.semaphore_signal(barrier, inc=1, device_id={"za": lax.rem(z + d, nz)}, device_id_type=MESH)
    for f in range(1, ny):
        pl.semaphore_signal(barrier, inc=1, device_id={"yb": lax.rem(y + f, ny)}, device_id_type=MESH)
    for e in range(1, nx):
        pl.semaphore_signal(barrier, inc=1, device_id={"xb": lax.rem(x + e, nx)}, device_id_type=MESH)
    for e in range(1, nc):
        pl.semaphore_signal(barrier, inc=1, device_id={"cb": other}, device_id_type=MESH)
    pl.semaphore_wait(barrier, nz + ny + nx + nc - 4)

    def tokens(zz, yy):
        return pl.ds(pl.multiple_of((zz * ny + yy) * tok, tok), tok)

    def kv_parts(zz, yy):
        at = tokens(zz, yy)
        return [kk.at[at]] + [vx.at[at, 2 * h * VD : (2 * h + 1) * VD] for h in range(heads)]

    def kv_sources(zp):
        base = zp * own
        return [k_hbm.at[:, pl.ds(pl.multiple_of(base, 128), own)]] + [
            v_hbm.at[:, pl.ds(pl.multiple_of(base + h * VD, 128), VD)] for h in range(heads)
        ]

    def q_source(zp):
        return q_hbm.at[:, pl.ds(pl.multiple_of(zp * own, 128), own)]

    nkv = 1 + heads

    def qkv_copies(d):
        zp = lax.rem(z + d, nz)
        pairs = list(zip(kv_sources(zp), kv_parts(z, y))) + [(q_source(zp), qs.at[z])]
        return [remote(s, t, qz_s.at[i, d], qz_r.at[i, z], za=zp) for i, (s, t) in enumerate(pairs)]

    def qkv_take(zp):
        pairs = list(zip(kv_sources(z), kv_parts(zp, y))) + [(q_source(z), qs.at[zp])]
        return [remote(s, t, qz_s.at[i, 0], qz_r.at[i, zp], za=zp) for i, (s, t) in enumerate(pairs)]

    def kv_pass(d, f):
        zp, yp = lax.rem(z + d, nz), lax.rem(y + f, ny)
        to = kv_parts(zp, y)
        fro = to if d else kv_sources(z)
        return [remote(s, t, ky_s.at[i, d, f], ky_r.at[i, zp, y], yb=yp) for i, (s, t) in enumerate(zip(fro, to))]

    def kv_take(zp, yp):
        to = kv_parts(zp, yp)
        return [remote(t, t, ky_s.at[i, 0, 0], ky_r.at[i, zp, yp], yb=yp) for i, t in enumerate(to)]

    mats = (gate_hbm, up_hbm, down_hbm)

    def place(m, xx, zz, yy, start=0, size=hid):
        at = zz * ny + yy
        r = pl.ds(pl.multiple_of(xx * hid + start, 8), size)
        if aligned:
            return w.at[m, r, pl.ds(pl.multiple_of(at * depth, depth), depth)]
        return wp.at[at, m, r]

    every = slice(None)

    def w_copies(d):
        zp = lax.rem(z + d, nz)
        return [
            remote(a.at[pl.ds(pl.multiple_of(zp * hid, 8), hid)], place(m, x, z, y), wz_s.at[m, d], wz_r.at[m, z], za=zp)
            for m, a in enumerate(mats)
        ]

    def w_local():
        return [
            pltpu.make_async_copy(a.at[pl.ds(pl.multiple_of(z * hid, 8), hid)], place(m, x, z, y), wl_s.at[m])
            for m, a in enumerate(mats)
        ]

    def w_x(d, e):
        zp, xp = lax.rem(z + d, nz), lax.rem(x + e, nx)
        at = place(every, x, zp, y)
        return remote(at, at, wx_s.at[d, e], wx_r.at[zp, x], xb=xp)

    def w_y(d, f):
        zp, yp = lax.rem(z + d, nz), lax.rem(y + f, ny)
        at = place(every, x, zp, y)
        return remote(at, at, wy_s.at[d, f], wy_r.at[zp, y], yb=yp)

    def w_xy(d, e, f):
        zp, xp, yp = lax.rem(z + d, nz), lax.rem(x + e, nx), lax.rem(y + f, ny)
        at = place(every, xp, zp, y, 0, cut)
        return remote(at, at, wxy_s.at[d, e, f], wxy_r.at[zp, xp, y], yb=yp)

    def w_yx(d, f, e):
        zp, xp, yp = lax.rem(z + d, nz), lax.rem(x + e, nx), lax.rem(y + f, ny)
        at = place(every, x, zp, yp, cut, hid - cut)
        return remote(at, at, wyx_s.at[d, f, e], wyx_r.at[zp, yp, x], xb=xp)

    def w_spread_x(d):
        for e in range(1, nx):
            w_x(d, e).start()

    def w_spread_y(d):
        for f in range(1, ny):
            w_y(d, f).start()

    def w_take(d):
        zp = lax.rem(z + d, nz)
        for m, a in enumerate(mats):
            remote(a.at[pl.ds(0, hid)], place(m, x, zp, y), wz_s.at[m, 0], wz_r.at[m, zp], za=zp).wait_recv()

    def w_turn(d):
        zp = lax.rem(z + d, nz)
        for e in range(1, nx):
            xp = lax.rem(x + e, nx)
            at = place(every, xp, zp, y)
            remote(at, at, wx_s.at[d, e], wx_r.at[zp, xp], xb=xp).wait_recv()
            for f in range(1, ny):
                w_xy(d, e, f).start()
        for f in range(1, ny):
            yp = lax.rem(y + f, ny)
            at = place(every, x, zp, yp)
            remote(at, at, wy_s.at[d, f], wy_r.at[zp, yp], yb=yp).wait_recv()
            for e in range(1, nx):
                w_yx(d, f, e).start()

    def w_done():
        for d in range(nz):
            zp = lax.rem(z + d, nz)
            for e in range(1, nx):
                xp = lax.rem(x + e, nx)
                for f in range(1, ny):
                    yp = lax.rem(y + f, ny)
                    at = place(every, xp, zp, yp, 0, cut)
                    remote(at, at, wxy_s.at[d, e, f], wxy_r.at[zp, xp, yp], yb=yp).wait_recv()
                    at = place(every, xp, zp, yp, cut, hid - cut)
                    remote(at, at, wyx_s.at[d, f, e], wyx_r.at[zp, yp, xp], xb=xp).wait_recv()
        if not aligned:
            for at in range(nz * ny):
                copy = pltpu.make_async_copy(wp.at[at], stage, st_s)
                copy.start()
                copy.wait()
                for m in range(3):
                    w[m, :, at * depth : (at + 1) * depth] = stage[m]

    for d in range(nz - 1, 0, -1):
        for copy in qkv_copies(d):
            copy.start()
    for f in range(1, ny):
        for copy in kv_pass(0, f):
            copy.start()
    locals_in = [
        pltpu.make_async_copy(s, t, in_s.at[i])
        for i, (s, t) in enumerate(
            list(zip(kv_sources(z), kv_parts(z, y))) + [(q_source(z), qs.at[z]), (ow_hbm, ow), (res_hbm, res)]
        )
    ]
    for copy in w_local() + locals_in:
        copy.start()
    for h in range(heads):
        vx[:, (2 * h + 1) * VD : (2 * h + 2) * VD] = jnp.ones((vx.shape[0], VD), jnp.bfloat16)
    for copy in w_local():
        copy.wait()
    w_spread_x(0)
    w_spread_y(0)
    for copy in locals_in:
        copy.wait()
    for d in range(1, nz):
        zp = lax.rem(z + d, nz)
        with jax.named_scope(f"qkv{d}"):
            for copy in qkv_take(zp):
                copy.wait_recv()
        for f in range(1, ny):
            for copy in kv_pass(d, f):
                copy.start()
    if nz > 1:
        for copy in w_copies(nz - 1):
            copy.start()
    for d in range(nz):
        zp = lax.rem(z + d, nz)
        for f in range(1, ny):
            with jax.named_scope(f"kv{d}"):
                for copy in kv_take(zp, lax.rem(y + f, ny)):
                    copy.wait_recv()
    with jax.named_scope("turn0"):
        w_turn(0)

    scale = LOG2E / math.sqrt(DH)
    block_rows = osend.shape[1]
    per = tok // block_rows

    def o_copy(i):
        zq = lax.rem(z + 1 + i // per, nz)
        off = pl.multiple_of(lax.rem(i, per) * block_rows, block_rows)
        to = att.at[pl.ds(off, block_rows), pl.ds(pl.multiple_of(z * own, 128), own)]
        return remote(osend.at[i], to, o_s.at[i], o_r.at[z, lax.rem(i, per)], za=zq)

    def block(i, carry):
        zq = lax.rem(z + 1 + i // per, nz)
        off = pl.multiple_of(lax.rem(i, per) * block_rows, block_rows)
        for h in range(heads):
            cols = slice(h * VD, (h + 1) * VD)
            q = qs[zq, pl.ds(off, block_rows), cols]
            lane = lax.broadcasted_iota(jnp.int32, q.shape, 1)
            maps = []
            for half in range(2):
                qc = jnp.where((lane >= DH) if half else (lane < DH), q, jnp.zeros_like(q))
                s = lax.dot_general(
                    qc, kk[:, cols], (((1,), (1,)), ((), ())), preferred_element_type=jnp.float32
                )
                top = jnp.max(s, axis=-1, keepdims=True)
                e = jnp.exp2((s - top) * scale).astype(jnp.bfloat16)
                o = jnp.dot(
                    e, vx[:, 2 * h * VD : (2 * h + 2) * VD], preferred_element_type=jnp.float32
                )
                maps.append(o[:, :VD] / o[:, VD:])
            mixed = maps[0] - lam_ref[z * heads + h] * maps[1]
            norm = lax.rsqrt(jnp.mean(mixed * mixed, axis=-1, keepdims=True) + 1e-06)
            osend[i, :, cols] = (mixed * norm * gain_ref[...]).astype(jnp.bfloat16)

        @pl.when(zq != z)
        def _():
            o_copy(i).start()

        if nz > 1:
            @pl.when(i == nz * per * 6 // 8)
            def _():
                with jax.named_scope("take1"):
                    w_take(1)
                    w_spread_x(1)
                    w_spread_y(1)

        return carry

    lax.fori_loop(0, nz * per, block, 0)
    for j in range(per):
        att[j * block_rows : (j + 1) * block_rows, pl.ds(pl.multiple_of(z * own, 128), own)] = osend[(nz - 1) * per + j]
    if nz > 2:
        for copy in w_copies(1):
            copy.start()
    for d in range(1, nz):
        zp = lax.rem(z + d, nz)
        with jax.named_scope(f"o_wait{d}"):
            for j in range(per):
                to = att.at[pl.ds(j * block_rows, block_rows), pl.ds(pl.multiple_of(zp * own, 128), own)]
                remote(osend.at[j], to, o_s.at[j], o_r.at[zp, j], za=zp).wait_recv()

    def split(part):
        if nc == 1:
            return part, None
        low, high = part[:rows], part[rows:]
        return jnp.where(c == 0, low, high), jnp.where(c == 0, high, low)

    def oc_copy(e):
        return remote(oc_send.at[e], oc_recv.at[e], oc_s.at[e], oc_r.at[e], cb=other)

    def ox_copy(e):
        return remote(ox_send.at[e], ox_recv.at[e], ox_s.at[e], ox_r.at[e], xb=lax.rem(x + e, nx))

    ring = list(range(1, nx)) + [0]
    for e in ring:
        xp = lax.rem(x + e, nx)
        part = jnp.dot(
            att[pl.ds(pl.multiple_of(xp * pair, 8), pair)], ow[...], preferred_element_type=jnp.float32
        )
        keep, send = split(part)
        om[e] = keep
        if nc > 1:
            oc_send[e] = send.astype(jnp.bfloat16)
            oc_copy(e).start()
    for e in ring:
        total = om[e]
        if nc > 1:
            oc_copy(e).wait_recv()
            total = total + oc_recv[e].astype(jnp.float32)
        if e:
            ox_send[e] = total.astype(jnp.bfloat16)
            ox_copy(e).start()
    for d in range(nz - 2, 1, -1):
        for copy in w_copies(d):
            copy.start()
    if nz > 2:
        with jax.named_scope("take_third"):
            w_take(nz - 1)
            w_spread_x(nz - 1)
            w_spread_y(nz - 1)
    if nz > 1:
        with jax.named_scope("turn1"):
            w_turn(1)
    after = res[...].astype(jnp.float32) + total
    for e in range(1, nx):
        ox_copy(e).wait_recv()
        after = after + ox_recv[e].astype(jnp.float32)
    om[0] = after
    row_scale = lax.rsqrt(jnp.mean(after * after, axis=-1, keepdims=True) + 1e-06)

    def slot(zp, cc):
        return got.at[zp, pl.ds(pl.multiple_of(cc * rows, 8), rows)]

    half = max(nz // 2, 1)
    outer = jnp.logical_or(z == 0, z == nz - 1)
    gate_way = jnp.logical_or(z == half - 1, z == half)

    def ag_z(zp, j, to):
        return remote(slot(zp, c), slot(zp, c), az_s.at[zp, j], az_r.at[zp], za=to)

    def near(j):
        return z // half * half + lax.rem(z + j, half)

    def ag_c(zp):
        return remote(slot(zp, c), slot(zp, c), ac_s.at[zp], ac_r.at[zp], cb=other)

    def rs_c(zp):
        return remote(c_send.at[zp], c_recv.at[zp], rc_s.at[zp], rc_r.at[zp], cb=other)

    inward = jnp.where(z < half, z + 1, z - 1)

    def same(zp):
        return z // half == zp // half

    joined = (nz - half) // 2

    def apart(zp):
        return jnp.where(zp < half, half - 1 - zp, zp - half) >= joined

    def at_once(zp):
        return jnp.logical_or(same(zp), jnp.logical_or(outer, apart(zp)))

    def straight(zp):
        return jnp.logical_or(same(zp), jnp.logical_or(gate_way, apart(zp)))

    def rs_z(zp):
        return remote(z_send.at[zp], z_recv.at[z], rz_s.at[zp], rz_r.at[z], za=zp)

    def rs_in(zp):
        return remote(z_send.at[zp], t_recv.at[zp], rz_s.at[zp], rt_r.at[zp], za=inward)

    def rs_act(zp, act):
        @pl.when(straight(zp))
        def _():
            act(rs_z(zp))

        if nz > 2:
            @pl.when(jnp.logical_not(straight(zp)))
            def _():
                act(rs_in(zp))

    got[z, pl.ds(pl.multiple_of(c * rows, 8), rows)] = (after * row_scale * ngain_ref[...]).astype(jnp.bfloat16)

    def onward(zp, act):
        if half > 1:
            @pl.when(gate_way)
            def _():
                for j in range(1, half):
                    act(ag_z(zp, j, near(j)))

    def own_ways(act):
        if nz > 1:
            act(ag_z(z, 0, jnp.where(z < half, half, half - 1)))
        for j in range(1, half):
            act(ag_z(z, j, near(j)))

    def own_near():
        for j in range(1, half):
            ag_z(z, j, near(j)).start()

    if half > 1:
        pl.when(outer)(own_near)
    if nz > 1:
        ag_z(z, 0, jnp.where(z < half, half, half - 1)).start()
    if half > 1:
        pl.when(jnp.logical_not(outer))(own_near)
    if nc > 1:
        ag_c(z).start()

    def pass_on(k):
        zp = across_first(z, k, nz)
        ag_z(zp, 0, zp).wait_recv()
        if k < nz - half:
            onward(zp, lambda copy: copy.start())
        if nc > 1:
            ag_c(zp).start()

    contract = (((1,), (1,)), ((), ()))

    def compute(k):
        zp = across_first(z, k, nz)
        if nc > 1:
            remote(slot(zp, other), slot(zp, other), ac_s.at[zp], ac_r.at[zp], cb=other).wait_recv()
        tokens_in = got[zp]
        gate = lax.dot_general(tokens_in, w[0], contract, preferred_element_type=jnp.float32)
        up = lax.dot_general(tokens_in, w[1], contract, preferred_element_type=jnp.float32)
        hidden = (jax.nn.silu(gate) * up).astype(jnp.bfloat16)
        keep, send = split(jnp.dot(hidden, w[2], preferred_element_type=jnp.float32))
        mine[zp] = keep
        if nc > 1:
            c_send[zp] = send.astype(jnp.bfloat16)
            rs_c(zp).start()

    def finish(k):
        zp = across_first(z, k, nz)
        total = mine[zp]
        if nc > 1:
            rs_c(zp).wait_recv()
            total = total + c_recv[zp].astype(jnp.float32)
        mine[zp] = total
        if k < nz - 1:
            @pl.when(at_once(zp))
            def _():
                z_send[zp] = total.astype(jnp.bfloat16)
                rs_act(zp, lambda copy: copy.start())
        return total

    def gather_in(k):
        zp = across_first(z, k, nz)

        @pl.when(jnp.logical_not(outer))
        def _():
            rs_in(zp).wait_recv()
            z_send[zp] = (mine[zp] + t_recv[zp].astype(jnp.float32)).astype(jnp.bfloat16)
            rs_act(zp, lambda copy: copy.start())

    if nz > 2:
        with jax.named_scope("turn_third"):
            w_turn(nz - 1)
    for d in range(2, nz - 1):
        with jax.named_scope(f"take{d}"):
            w_take(d)
            w_spread_x(d)
            w_spread_y(d)
    def pass_across():
        for k in range(nz - half):
            with jax.named_scope(f"pass{k}"):
                pass_on(k)

    if half > 1:
        pl.when(gate_way)(pass_across)
    for d in range(2, nz - 1):
        with jax.named_scope(f"turn{d}"):
            w_turn(d)
    for k in range(nz - half, nz - 1):
        with jax.named_scope(f"pass{k}"):
            pass_on(k)
    with jax.named_scope("w_done"):
        w_done()
    order = list(range(max(nz - half - 1, 0))) + list(range(nz - half, nz - 1)) + list(range(max(nz - half - 1, 0), nz - half)) + [nz - 1]
    for i, k in enumerate(order):
        if k < nz - half:
            late = functools.partial(pass_on, k)
            with jax.named_scope(f"late_pass{k}"):
                if half > 1:
                    pl.when(jnp.logical_not(gate_way))(late)
                else:
                    late()
        with jax.named_scope(f"compute{k}"):
            compute(k)
        if i:
            with jax.named_scope(f"finish{order[i - 1]}"):
                finish(order[i - 1])
    finish(order[-1])
    if nz > 2:
        for k in range(joined):
            with jax.named_scope(f"gather_in{k}"):
                gather_in(k)
    for k in range(nz - 2, -1, -1):
        zp = across_first(z, k, nz)
        with jax.named_scope(f"rz{k}"):
            @pl.when(jnp.logical_or(jnp.logical_or(same(zp), apart(z)), jnp.logical_or(zp == half - 1, zp == half)))
            def _():
                remote(z_send.at[zp], z_recv.at[zp], rz_s.at[zp], rz_r.at[zp], za=zp).wait_recv()
                mine[z] = mine[z] + z_recv[zp].astype(jnp.float32)
    total = mine[z]
    out[...] = (om[0] + 0.5 * total).astype(jnp.bfloat16)

    for d in range(1, nz):
        for copy in qkv_copies(d) + w_copies(d):
            copy.wait_send()
    for d in range(nz):
        for f in range(1, ny):
            for copy in kv_pass(d, f):
                copy.wait_send()
            w_y(d, f).wait_send()
        for e in range(1, nx):
            w_x(d, e).wait_send()
            for f in range(1, ny):
                w_xy(d, e, f).wait_send()
                w_yx(d, f, e).wait_send()
    for i in range((nz - 1) * per):
        o_copy(i).wait_send()
    for e in range(nx):
        if nc > 1:
            oc_copy(e).wait_send()
        if e:
            ox_copy(e).wait_send()
    own_ways(lambda copy: copy.wait_send())
    for k in range(nz):
        zp = across_first(z, k, nz)
        if k < nz - half:
            onward(zp, lambda copy: copy.wait_send())
        if k < nz - 1:
            rs_act(zp, lambda copy: copy.wait_send())
        if nc > 1:
            ag_c(zp).wait_send()
            rs_c(zp).wait_send()


def body(
    residual_in,
    queries,
    keys,
    values,
    mix_lambda,
    head_gain,
    out_weight,
    norm_gain,
    gate_weight,
    up_weight,
    down_weight,
):
    nz, ny, nx, nc = (lax.axis_size(name) for name in AXES)
    tok, width = queries.shape
    rows, model = residual_in.shape
    heads = mix_lambda.shape[0] // nz
    own = width // nz
    depth = down_weight.shape[1]
    hid = down_weight.shape[0] // nz
    aligned = depth % 128 == 0
    nsp = nz * ny
    block_rows = 2 * rows
    per = tok // block_rows
    vmem = pl.BlockSpec(memory_space=pltpu.VMEM)
    smem = pl.BlockSpec(memory_space=pltpu.SMEM)
    hbm = pl.BlockSpec(memory_space=pl.ANY)
    dma = pltpu.SemaphoreType.DMA
    bf16, f32 = jnp.bfloat16, jnp.float32
    parts = (8, 128) if aligned else (3, nx * hid, depth)
    return pl.pallas_call(
        functools.partial(layer_kernel, (nz, ny, nx, nc, heads, aligned)),
        out_shape=(
            jax.ShapeDtypeStruct((rows, model), bf16),
            jax.ShapeDtypeStruct(parts if aligned else (nsp, *parts), bf16),
        ),
        in_specs=[smem, vmem, vmem] + [hbm] * 8,
        out_specs=(vmem, hbm),
        scratch_shapes=[
            pltpu.VMEM((nz, tok, own), bf16),
            pltpu.VMEM((nsp * tok, own), bf16),
            pltpu.VMEM((nsp * tok, 2 * own), bf16),
            pltpu.VMEM((nz * per, block_rows, own), bf16),
            pltpu.VMEM((tok, width), bf16),
            pltpu.VMEM((width, model), bf16),
            pltpu.VMEM((rows, model), bf16),
            pltpu.VMEM((3, nx * hid, model), bf16),
            pltpu.VMEM(parts, bf16),
            pltpu.VMEM((nx, rows, model), f32),
            pltpu.VMEM((nx, rows, model), bf16),
            pltpu.VMEM((nx, rows, model), bf16),
            pltpu.VMEM((nx, rows, model), bf16),
            pltpu.VMEM((nx, rows, model), bf16),
            pltpu.VMEM((nz, nc * rows, model), bf16),
            pltpu.VMEM((nz, rows, model), f32),
            pltpu.VMEM((nz, rows, model), bf16),
            pltpu.VMEM((nz, rows, model), bf16),
            pltpu.VMEM((nz, rows, model), bf16),
            pltpu.VMEM((nz, rows, model), bf16),
            pltpu.VMEM((nz, rows, model), bf16),
            dma((heads + 4,)), dma,
            dma((heads + 2, nz)), dma((heads + 2, nz)),
            dma((heads + 1, nz, ny)), dma((heads + 1, nz, ny)),
            dma((3,)),
            dma((3, nz)), dma((3, nz)),
            dma((nz, nx)), dma((nz, nx)),
            dma((nz, ny)), dma((nz, ny)),
            dma((nz, nx, ny)), dma((nz, nx, ny)),
            dma((nz, ny, nx)), dma((nz, ny, nx)),
            dma((nz * per,)), dma((nz, per)),
            dma((nx,)), dma((nx,)),
            dma((nx,)), dma((nx,)),
            dma((nz, max(nz // 2, 1))), dma((nz,)),
            dma((nz,)), dma((nz,)),
            dma((nz,)), dma((nz,)),
            dma((nz,)), dma((nz,)), dma((nz,)),
        ],
        compiler_params=pltpu.CompilerParams(
            collective_id=1, has_side_effects=True, vmem_limit_bytes=62 * 1024 * 1024
        ),
    )(
        mix_lambda,
        head_gain.reshape(1, VD),
        norm_gain.reshape(1, model),
        residual_in,
        queries,
        keys,
        values,
        out_weight,
        gate_weight.T,
        up_weight.T,
        down_weight,
    )[0]


def solution(mesh):
    sp, tp = mesh.shape["sp"], mesh.shape["tp"]

    def run(*args):
        heads_local = args[4].shape[0] // tp
        za = math.gcd(heads_local, sp)
        nc = math.gcd(tp, 2)
        cut = Mesh(mesh.devices.reshape(za, sp // za, tp // nc, nc), AXES)
        s, t = ("za", "yb"), ("xb", "cb")
        return jax.shard_map(
            body,
            mesh=cut,
            in_specs=(
                P(AXES, None),
                P(s, t),
                P(s, t),
                P(s, t),
                P(t),
                P(),
                P(t, None),
                P(),
                P(s, t),
                P(s, t),
                P(t, s),
            ),
            out_specs=P(AXES, None),
            check_vma=False,
        )(*args)

    return run
```

```python
import functools
import math

import jax
import jax.numpy as jnp
from jax import lax
from jax.experimental import pallas as pl
from jax.experimental.pallas import tpu as pltpu
from jax.sharding import Mesh, PartitionSpec as P

DH = 64
VD = 128
LOG2E = 1.4426950408889634

MESH = pl.DeviceIdType.MESH
AXES = ("za", "yb", "xb", "cb")


def remote(src, dst, send, recv, **where):
    return pltpu.make_async_remote_copy(
        src_ref=src, dst_ref=dst, send_sem=send, recv_sem=recv, device_id=where, device_id_type=MESH
    )


def across_first(z, k, nz):
    half = max(nz // 2, 1)
    if k < nz - half:
        return jnp.where(z < half, half + k, half - 1 - k)
    return z // half * half + lax.rem(z + 1 + k - (nz - half), half)


def layer_kernel(n, lam_ref, gain_ref, ngain_ref, res_hbm, q_hbm, k_hbm, v_hbm, ow_hbm, gate_in, up_in, down_hbm,
                 out, wp,
                 qs, kk, vx, osend, att, ow, res, w, stage, raw, turned, om, oc_send, oc_recv, ox_send, ox_recv,
                 got, mine, c_send, c_recv, z_send, z_recv, t_recv,
                 in_s, st_s, raw_s, qz_s, qz_r, ky_s, ky_r, wl_s, wz_s, wz_r, wx_s, wx_r, wy_s, wy_r,
                 wxy_s, wxy_r, wyx_s, wyx_r, o_s, o_r, oc_s, oc_r, ox_s, ox_r,
                 az_s, az_r, ac_s, ac_r, rc_s, rc_r, rz_s, rz_r, rt_r):
    nz, ny, nx, nc, heads, aligned = n
    z, y, x, c = (lax.axis_index(name) for name in AXES)
    other = nc - 1 - c
    tok, own = qs.shape[1:]
    rows, model = res.shape
    pair = nc * rows
    hid, depth = down_hbm.shape[0] // nz, down_hbm.shape[1]
    turn_here = gate_in.shape != down_hbm.shape
    cut = hid // 16 * 8

    barrier = pltpu.get_barrier_semaphore()
    for d in range(1, nz):
        pl.semaphore_signal(barrier, inc=1, device_id={"za": lax.rem(z + d, nz)}, device_id_type=MESH)
    for f in range(1, ny):
        pl.semaphore_signal(barrier, inc=1, device_id={"yb": lax.rem(y + f, ny)}, device_id_type=MESH)
    for e in range(1, nx):
        pl.semaphore_signal(barrier, inc=1, device_id={"xb": lax.rem(x + e, nx)}, device_id_type=MESH)
    for e in range(1, nc):
        pl.semaphore_signal(barrier, inc=1, device_id={"cb": other}, device_id_type=MESH)
    pl.semaphore_wait(barrier, nz + ny + nx + nc - 4)

    def tokens(zz, yy):
        return pl.ds(pl.multiple_of((zz * ny + yy) * tok, tok), tok)

    def kv_parts(zz, yy):
        at = tokens(zz, yy)
        return [kk.at[at]] + [vx.at[at, 2 * h * VD : (2 * h + 1) * VD] for h in range(heads)]

    def kv_sources(zp):
        base = zp * own
        return [k_hbm.at[:, pl.ds(pl.multiple_of(base, 128), own)]] + [
            v_hbm.at[:, pl.ds(pl.multiple_of(base + h * VD, 128), VD)] for h in range(heads)
        ]

    def q_source(zp):
        return q_hbm.at[:, pl.ds(pl.multiple_of(zp * own, 128), own)]

    nkv = 1 + heads

    def qkv_copies(d):
        zp = lax.rem(z + d, nz)
        pairs = list(zip(kv_sources(zp), kv_parts(z, y))) + [(q_source(zp), qs.at[z])]
        return [remote(s, t, qz_s.at[i, d], qz_r.at[i, z], za=zp) for i, (s, t) in enumerate(pairs)]

    def qkv_take(zp):
        pairs = list(zip(kv_sources(z), kv_parts(zp, y))) + [(q_source(z), qs.at[zp])]
        return [remote(s, t, qz_s.at[i, 0], qz_r.at[i, zp], za=zp) for i, (s, t) in enumerate(pairs)]

    def kv_pass(d, f):
        zp, yp = lax.rem(z + d, nz), lax.rem(y + f, ny)
        to = kv_parts(zp, y)
        fro = to if d else kv_sources(z)
        return [remote(s, t, ky_s.at[i, d, f], ky_r.at[i, zp, y], yb=yp) for i, (s, t) in enumerate(zip(fro, to))]

    def kv_take(zp, yp):
        to = kv_parts(zp, yp)
        return [remote(t, t, ky_s.at[i, 0, 0], ky_r.at[i, zp, yp], yb=yp) for i, t in enumerate(to)]

    mats = (turned.at[0], turned.at[1], down_hbm) if turn_here else (gate_in, up_in, down_hbm)

    def place(m, xx, zz, yy, start=0, size=hid):
        at = zz * ny + yy
        r = pl.ds(pl.multiple_of(xx * hid + start, 8), size)
        if aligned:
            return w.at[m, r, pl.ds(pl.multiple_of(at * depth, depth), depth)]
        return wp.at[at, m, r]

    every = slice(None)

    def w_copies(d):
        zp = lax.rem(z + d, nz)
        return [
            remote(a.at[pl.ds(pl.multiple_of(zp * hid, 8), hid)], place(m, x, z, y), wz_s.at[m, d], wz_r.at[m, z], za=zp)
            for m, a in enumerate(mats)
        ]

    def w_local():
        return [
            pltpu.make_async_copy(a.at[pl.ds(pl.multiple_of(z * hid, 8), hid)], place(m, x, z, y), wl_s.at[m])
            for m, a in enumerate(mats)
            if m == 2 or not turn_here
        ]

    def w_x(d, e):
        zp, xp = lax.rem(z + d, nz), lax.rem(x + e, nx)
        at = place(every, x, zp, y)
        return remote(at, at, wx_s.at[d, e], wx_r.at[zp, x], xb=xp)

    def w_y(d, f):
        zp, yp = lax.rem(z + d, nz), lax.rem(y + f, ny)
        at = place(every, x, zp, y)
        return remote(at, at, wy_s.at[d, f], wy_r.at[zp, y], yb=yp)

    def w_xy(d, e, f):
        zp, xp, yp = lax.rem(z + d, nz), lax.rem(x + e, nx), lax.rem(y + f, ny)
        at = place(every, xp, zp, y, 0, cut)
        return remote(at, at, wxy_s.at[d, e, f], wxy_r.at[zp, xp, y], yb=yp)

    def w_yx(d, f, e):
        zp, xp, yp = lax.rem(z + d, nz), lax.rem(x + e, nx), lax.rem(y + f, ny)
        at = place(every, x, zp, yp, cut, hid - cut)
        return remote(at, at, wyx_s.at[d, f, e], wyx_r.at[zp, yp, x], xb=xp)

    def w_spread_x(d):
        for e in range(1, nx):
            w_x(d, e).start()

    def w_spread_y(d):
        for f in range(1, ny):
            w_y(d, f).start()

    def w_take(d):
        zp = lax.rem(z + d, nz)
        for m, a in enumerate(mats):
            remote(a.at[pl.ds(0, hid)], place(m, x, zp, y), wz_s.at[m, 0], wz_r.at[m, zp], za=zp).wait_recv()

    def w_turn(d):
        zp = lax.rem(z + d, nz)
        for e in range(1, nx):
            xp = lax.rem(x + e, nx)
            at = place(every, xp, zp, y)
            remote(at, at, wx_s.at[d, e], wx_r.at[zp, xp], xb=xp).wait_recv()
            for f in range(1, ny):
                w_xy(d, e, f).start()
        for f in range(1, ny):
            yp = lax.rem(y + f, ny)
            at = place(every, x, zp, yp)
            remote(at, at, wy_s.at[d, f], wy_r.at[zp, yp], yb=yp).wait_recv()
            for e in range(1, nx):
                w_yx(d, f, e).start()

    def w_done():
        for d in range(nz):
            zp = lax.rem(z + d, nz)
            for e in range(1, nx):
                xp = lax.rem(x + e, nx)
                for f in range(1, ny):
                    yp = lax.rem(y + f, ny)
                    at = place(every, xp, zp, yp, 0, cut)
                    remote(at, at, wxy_s.at[d, e, f], wxy_r.at[zp, xp, yp], yb=yp).wait_recv()
                    at = place(every, xp, zp, yp, cut, hid - cut)
                    remote(at, at, wyx_s.at[d, f, e], wyx_r.at[zp, yp, xp], xb=xp).wait_recv()
        if not aligned:
            for at in range(nz * ny):
                copy = pltpu.make_async_copy(wp.at[at], stage, st_s)
                copy.start()
                copy.wait()
                for m in range(3):
                    w[m, :, at * depth : (at + 1) * depth] = stage[m]

    for d in range(nz - 1, 0, -1):
        for copy in qkv_copies(d):
            copy.start()
    for f in range(1, ny):
        for copy in kv_pass(0, f):
            copy.start()
    locals_in = [
        pltpu.make_async_copy(s, t, in_s.at[i])
        for i, (s, t) in enumerate(
            list(zip(kv_sources(z), kv_parts(z, y))) + [(q_source(z), qs.at[z]), (ow_hbm, ow), (res_hbm, res)]
        )
    ]
    raws = [pltpu.make_async_copy(a, raw.at[i], raw_s.at[i]) for i, a in enumerate((gate_in, up_in))] if turn_here else []
    for copy in raws + w_local() + locals_in:
        copy.start()
    for h in range(heads):
        vx[:, (2 * h + 1) * VD : (2 * h + 2) * VD] = jnp.ones((vx.shape[0], VD), jnp.bfloat16)
    for i, copy in enumerate(raws):
        copy.wait()
        turned[i] = raw[i].T
        place(i, x, z, y)[...] = turned[i, pl.ds(pl.multiple_of(z * hid, 8), hid)]
    for copy in w_local():
        copy.wait()
    w_spread_x(0)
    w_spread_y(0)
    for copy in locals_in:
        copy.wait()
    for d in range(1, nz):
        zp = lax.rem(z + d, nz)
        with jax.named_scope(f"qkv{d}"):
            for copy in qkv_take(zp):
                copy.wait_recv()
        for f in range(1, ny):
            for copy in kv_pass(d, f):
                copy.start()
    if nz > 1:
        for copy in w_copies(nz - 1):
            copy.start()
    for d in range(nz):
        zp = lax.rem(z + d, nz)
        for f in range(1, ny):
            with jax.named_scope(f"kv{d}"):
                for copy in kv_take(zp, lax.rem(y + f, ny)):
                    copy.wait_recv()
    with jax.named_scope("turn0"):
        w_turn(0)

    scale = LOG2E / math.sqrt(DH)
    block_rows = osend.shape[1]
    per = tok // block_rows

    def o_copy(i):
        zq = lax.rem(z + 1 + i // per, nz)
        off = pl.multiple_of(lax.rem(i, per) * block_rows, block_rows)
        to = att.at[pl.ds(off, block_rows), pl.ds(pl.multiple_of(z * own, 128), own)]
        return remote(osend.at[i], to, o_s.at[i], o_r.at[z, lax.rem(i, per)], za=zq)

    def block(i, carry):
        zq = lax.rem(z + 1 + i // per, nz)
        off = pl.multiple_of(lax.rem(i, per) * block_rows, block_rows)
        for h in range(heads):
            cols = slice(h * VD, (h + 1) * VD)
            q = qs[zq, pl.ds(off, block_rows), cols]
            lane = lax.broadcasted_iota(jnp.int32, q.shape, 1)
            maps = []
            for half in range(2):
                qc = jnp.where((lane >= DH) if half else (lane < DH), q, jnp.zeros_like(q))
                s = lax.dot_general(
                    qc, kk[:, cols], (((1,), (1,)), ((), ())), preferred_element_type=jnp.float32
                )
                top = jnp.max(s, axis=-1, keepdims=True)
                e = jnp.exp2((s - top) * scale).astype(jnp.bfloat16)
                o = jnp.dot(
                    e, vx[:, 2 * h * VD : (2 * h + 2) * VD], preferred_element_type=jnp.float32
                )
                maps.append(o[:, :VD] / o[:, VD:])
            mixed = maps[0] - lam_ref[z * heads + h] * maps[1]
            norm = lax.rsqrt(jnp.mean(mixed * mixed, axis=-1, keepdims=True) + 1e-06)
            osend[i, :, cols] = (mixed * norm * gain_ref[...]).astype(jnp.bfloat16)

        @pl.when(zq != z)
        def _():
            o_copy(i).start()

        if nz > 1:
            @pl.when(i == nz * per * 6 // 8)
            def _():
                with jax.named_scope("take1"):
                    w_take(1)
                    w_spread_x(1)
                    w_spread_y(1)

        return carry

    lax.fori_loop(0, nz * per, block, 0)
    for j in range(per):
        att[j * block_rows : (j + 1) * block_rows, pl.ds(pl.multiple_of(z * own, 128), own)] = osend[(nz - 1) * per + j]
    for d in range(1, nz):
        zp = lax.rem(z + d, nz)
        with jax.named_scope(f"o_wait{d}"):
            for j in range(per):
                to = att.at[pl.ds(j * block_rows, block_rows), pl.ds(pl.multiple_of(zp * own, 128), own)]
                remote(osend.at[j], to, o_s.at[j], o_r.at[zp, j], za=zp).wait_recv()

    if nz > 2:
        for copy in w_copies(1):
            copy.start()
    for d in range(nz - 2, 1, -1):
        for copy in w_copies(d):
            copy.start()

    def split(part):
        if nc == 1:
            return part, None
        low, high = part[:rows], part[rows:]
        return jnp.where(c == 0, low, high), jnp.where(c == 0, high, low)

    def oc_copy(e):
        return remote(oc_send.at[e], oc_recv.at[e], oc_s.at[e], oc_r.at[e], cb=other)

    def ox_copy(e):
        return remote(ox_send.at[e], ox_recv.at[e], ox_s.at[e], ox_r.at[e], xb=lax.rem(x + e, nx))

    ring = list(range(1, nx)) + [0]
    for e in ring:
        xp = lax.rem(x + e, nx)
        part = jnp.dot(
            att[pl.ds(pl.multiple_of(xp * pair, 8), pair)], ow[...], preferred_element_type=jnp.float32
        )
        keep, send = split(part)
        om[e] = keep
        if nc > 1:
            oc_send[e] = send.astype(jnp.bfloat16)
            oc_copy(e).start()
    for e in ring:
        total = om[e]
        if nc > 1:
            oc_copy(e).wait_recv()
            total = total + oc_recv[e].astype(jnp.float32)
        if e:
            ox_send[e] = total.astype(jnp.bfloat16)
            ox_copy(e).start()
    if nz > 2:
        with jax.named_scope("take_third"):
            w_take(nz - 1)
            w_spread_x(nz - 1)
            w_spread_y(nz - 1)
    if nz > 1:
        with jax.named_scope("turn1"):
            w_turn(1)
    after = res[...].astype(jnp.float32) + total
    for e in range(1, nx):
        ox_copy(e).wait_recv()
        after = after + ox_recv[e].astype(jnp.float32)
    om[0] = after
    row_scale = lax.rsqrt(jnp.mean(after * after, axis=-1, keepdims=True) + 1e-06)

    def slot(zp, cc):
        return got.at[zp, pl.ds(pl.multiple_of(cc * rows, 8), rows)]

    half = max(nz // 2, 1)
    outer = jnp.logical_or(z == 0, z == nz - 1)
    gate_way = jnp.logical_or(z == half - 1, z == half)

    def ag_z(zp, j, to):
        return remote(slot(zp, c), slot(zp, c), az_s.at[zp, j], az_r.at[zp], za=to)

    def near(j):
        return z // half * half + lax.rem(z + j, half)

    def ag_c(zp):
        return remote(slot(zp, c), slot(zp, c), ac_s.at[zp], ac_r.at[zp], cb=other)

    def rs_c(zp):
        return remote(c_send.at[zp], c_recv.at[zp], rc_s.at[zp], rc_r.at[zp], cb=other)

    inward = jnp.where(z < half, z + 1, z - 1)

    def same(zp):
        return z // half == zp // half

    joined = (nz - half) // 2

    def apart(zp):
        return jnp.where(zp < half, half - 1 - zp, zp - half) >= joined

    def at_once(zp):
        return jnp.logical_or(same(zp), jnp.logical_or(outer, apart(zp)))

    def straight(zp):
        return jnp.logical_or(same(zp), jnp.logical_or(gate_way, apart(zp)))

    def rs_z(zp):
        return remote(z_send.at[zp], z_recv.at[z], rz_s.at[zp], rz_r.at[z], za=zp)

    def rs_in(zp):
        return remote(z_send.at[zp], t_recv.at[zp], rz_s.at[zp], rt_r.at[zp], za=inward)

    def rs_act(zp, act):
        @pl.when(straight(zp))
        def _():
            act(rs_z(zp))

        if nz > 2:
            @pl.when(jnp.logical_not(straight(zp)))
            def _():
                act(rs_in(zp))

    got[z, pl.ds(pl.multiple_of(c * rows, 8), rows)] = (after * row_scale * ngain_ref[...]).astype(jnp.bfloat16)

    def onward(zp, act):
        if half > 1:
            @pl.when(gate_way)
            def _():
                for j in range(1, half):
                    act(ag_z(zp, j, near(j)))

    def own_ways(act):
        if nz > 1:
            act(ag_z(z, 0, jnp.where(z < half, half, half - 1)))
        for j in range(1, half):
            act(ag_z(z, j, near(j)))

    def own_near():
        for j in range(1, half):
            ag_z(z, j, near(j)).start()

    if half > 1:
        pl.when(outer)(own_near)
    if nz > 1:
        ag_z(z, 0, jnp.where(z < half, half, half - 1)).start()
    if half > 1:
        pl.when(jnp.logical_not(outer))(own_near)
    if nc > 1:
        ag_c(z).start()

    def pass_on(k):
        zp = across_first(z, k, nz)
        ag_z(zp, 0, zp).wait_recv()
        if k < nz - half:
            onward(zp, lambda copy: copy.start())
        if nc > 1:
            ag_c(zp).start()

    contract = (((1,), (1,)), ((), ()))

    def compute(k):
        zp = across_first(z, k, nz)
        if nc > 1:
            remote(slot(zp, other), slot(zp, other), ac_s.at[zp], ac_r.at[zp], cb=other).wait_recv()
        tokens_in = got[zp]
        gate = lax.dot_general(tokens_in, w[0], contract, preferred_element_type=jnp.float32)
        up = lax.dot_general(tokens_in, w[1], contract, preferred_element_type=jnp.float32)
        hidden = (jax.nn.silu(gate) * up).astype(jnp.bfloat16)
        keep, send = split(jnp.dot(hidden, w[2], preferred_element_type=jnp.float32))
        mine[zp] = keep
        if nc > 1:
            c_send[zp] = send.astype(jnp.bfloat16)
            rs_c(zp).start()

    def finish(k):
        zp = across_first(z, k, nz)
        total = mine[zp]
        if nc > 1:
            rs_c(zp).wait_recv()
            total = total + c_recv[zp].astype(jnp.float32)
        mine[zp] = total
        if k < nz - 1:
            @pl.when(at_once(zp))
            def _():
                z_send[zp] = total.astype(jnp.bfloat16)
                rs_act(zp, lambda copy: copy.start())
        return total

    def gather_in(k):
        zp = across_first(z, k, nz)

        @pl.when(jnp.logical_not(outer))
        def _():
            rs_in(zp).wait_recv()
            z_send[zp] = (mine[zp] + t_recv[zp].astype(jnp.float32)).astype(jnp.bfloat16)
            rs_act(zp, lambda copy: copy.start())

    if nz > 2:
        with jax.named_scope("turn_third"):
            w_turn(nz - 1)
    for d in range(2, nz - 1):
        with jax.named_scope(f"take{d}"):
            w_take(d)
            w_spread_x(d)
            w_spread_y(d)
    def pass_across():
        for k in range(nz - half):
            with jax.named_scope(f"pass{k}"):
                pass_on(k)

    if half > 1:
        pl.when(gate_way)(pass_across)
    for d in range(2, nz - 1):
        with jax.named_scope(f"turn{d}"):
            w_turn(d)
    for k in range(nz - half, nz - 1):
        with jax.named_scope(f"pass{k}"):
            pass_on(k)
    with jax.named_scope("w_done"):
        w_done()
    order = list(range(max(nz - half - 1, 0))) + list(range(nz - half, nz - 1)) + list(range(max(nz - half - 1, 0), nz - half)) + [nz - 1]
    for i, k in enumerate(order):
        if k < nz - half:
            late = functools.partial(pass_on, k)
            with jax.named_scope(f"late_pass{k}"):
                if half > 1:
                    pl.when(jnp.logical_not(gate_way))(late)
                else:
                    late()
        with jax.named_scope(f"compute{k}"):
            compute(k)
        if i:
            with jax.named_scope(f"finish{order[i - 1]}"):
                finish(order[i - 1])
    finish(order[-1])
    if nz > 2:
        for k in range(joined):
            with jax.named_scope(f"gather_in{k}"):
                gather_in(k)
    for k in range(nz - 2, -1, -1):
        zp = across_first(z, k, nz)
        with jax.named_scope(f"rz{k}"):
            @pl.when(jnp.logical_or(jnp.logical_or(same(zp), apart(z)), jnp.logical_or(zp == half - 1, zp == half)))
            def _():
                remote(z_send.at[zp], z_recv.at[zp], rz_s.at[zp], rz_r.at[zp], za=zp).wait_recv()
                mine[z] = mine[z] + z_recv[zp].astype(jnp.float32)
    total = mine[z]
    out[...] = (om[0] + 0.5 * total).astype(jnp.bfloat16)

    for d in range(1, nz):
        for copy in qkv_copies(d) + w_copies(d):
            copy.wait_send()
    for d in range(nz):
        for f in range(1, ny):
            for copy in kv_pass(d, f):
                copy.wait_send()
            w_y(d, f).wait_send()
        for e in range(1, nx):
            w_x(d, e).wait_send()
            for f in range(1, ny):
                w_xy(d, e, f).wait_send()
                w_yx(d, f, e).wait_send()
    for i in range((nz - 1) * per):
        o_copy(i).wait_send()
    for e in range(nx):
        if nc > 1:
            oc_copy(e).wait_send()
        if e:
            ox_copy(e).wait_send()
    own_ways(lambda copy: copy.wait_send())
    for k in range(nz):
        zp = across_first(z, k, nz)
        if k < nz - half:
            onward(zp, lambda copy: copy.wait_send())
        if k < nz - 1:
            rs_act(zp, lambda copy: copy.wait_send())
        if nc > 1:
            ag_c(zp).wait_send()
            rs_c(zp).wait_send()


def body(
    residual_in,
    queries,
    keys,
    values,
    mix_lambda,
    head_gain,
    out_weight,
    norm_gain,
    gate_weight,
    up_weight,
    down_weight,
):
    nz, ny, nx, nc = (lax.axis_size(name) for name in AXES)
    tok, width = queries.shape
    rows, model = residual_in.shape
    heads = mix_lambda.shape[0] // nz
    own = width // nz
    depth = down_weight.shape[1]
    hid = down_weight.shape[0] // nz
    aligned = depth % 128 == 0
    nsp = nz * ny
    block_rows = 2 * rows
    per = tok // block_rows
    vmem = pl.BlockSpec(memory_space=pltpu.VMEM)
    smem = pl.BlockSpec(memory_space=pltpu.SMEM)
    hbm = pl.BlockSpec(memory_space=pl.ANY)
    dma = pltpu.SemaphoreType.DMA
    bf16, f32 = jnp.bfloat16, jnp.float32
    parts = (8, 128) if aligned else (3, nx * hid, depth)
    turn_here = aligned and (nz * hid) % 128 == 0 and depth != nz * hid
    gate, up = (gate_weight, up_weight) if turn_here else (gate_weight.T, up_weight.T)
    raw = (2, *gate_weight.shape) if turn_here else (2, 8, 128)
    turned = (2, *down_weight.shape) if turn_here else (2, 8, 128)
    return pl.pallas_call(
        functools.partial(layer_kernel, (nz, ny, nx, nc, heads, aligned)),
        out_shape=(
            jax.ShapeDtypeStruct((rows, model), bf16),
            jax.ShapeDtypeStruct(parts if aligned else (nsp, *parts), bf16),
        ),
        in_specs=[smem, vmem, vmem] + [hbm] * 8,
        out_specs=(vmem, hbm),
        scratch_shapes=[
            pltpu.VMEM((nz, tok, own), bf16),
            pltpu.VMEM((nsp * tok, own), bf16),
            pltpu.VMEM((nsp * tok, 2 * own), bf16),
            pltpu.VMEM((nz * per, block_rows, own), bf16),
            pltpu.VMEM((tok, width), bf16),
            pltpu.VMEM((width, model), bf16),
            pltpu.VMEM((rows, model), bf16),
            pltpu.VMEM((3, nx * hid, model), bf16),
            pltpu.VMEM(parts, bf16),
            pltpu.VMEM(raw, bf16),
            pltpu.VMEM(turned, bf16),
            pltpu.VMEM((nx, rows, model), f32),
            pltpu.VMEM((nx, rows, model), bf16),
            pltpu.VMEM((nx, rows, model), bf16),
            pltpu.VMEM((nx, rows, model), bf16),
            pltpu.VMEM((nx, rows, model), bf16),
            pltpu.VMEM((nz, nc * rows, model), bf16),
            pltpu.VMEM((nz, rows, model), f32),
            pltpu.VMEM((nz, rows, model), bf16),
            pltpu.VMEM((nz, rows, model), bf16),
            pltpu.VMEM((nz, rows, model), bf16),
            pltpu.VMEM((nz, rows, model), bf16),
            pltpu.VMEM((nz, rows, model), bf16),
            dma((heads + 4,)), dma, dma((2,)),
            dma((heads + 2, nz)), dma((heads + 2, nz)),
            dma((heads + 1, nz, ny)), dma((heads + 1, nz, ny)),
            dma((3,)),
            dma((3, nz)), dma((3, nz)),
            dma((nz, nx)), dma((nz, nx)),
            dma((nz, ny)), dma((nz, ny)),
            dma((nz, nx, ny)), dma((nz, nx, ny)),
            dma((nz, ny, nx)), dma((nz, ny, nx)),
            dma((nz * per,)), dma((nz, per)),
            dma((nx,)), dma((nx,)),
            dma((nx,)), dma((nx,)),
            dma((nz, max(nz // 2, 1))), dma((nz,)),
            dma((nz,)), dma((nz,)),
            dma((nz,)), dma((nz,)),
            dma((nz,)), dma((nz,)), dma((nz,)),
        ],
        compiler_params=pltpu.CompilerParams(
            collective_id=1, has_side_effects=True, vmem_limit_bytes=62 * 1024 * 1024
        ),
    )(
        mix_lambda,
        head_gain.reshape(1, VD),
        norm_gain.reshape(1, model),
        residual_in,
        queries,
        keys,
        values,
        out_weight,
        gate,
        up,
        down_weight,
    )[0]


def solution(mesh):
    sp, tp = mesh.shape["sp"], mesh.shape["tp"]

    def run(*args):
        heads_local = args[4].shape[0] // tp
        za = math.gcd(heads_local, sp)
        nc = math.gcd(tp, 2)
        cut = Mesh(mesh.devices.reshape(za, sp // za, tp // nc, nc), AXES)
        s, t = ("za", "yb"), ("xb", "cb")
        return jax.shard_map(
            body,
            mesh=cut,
            in_specs=(
                P(AXES, None),
                P(s, t),
                P(s, t),
                P(s, t),
                P(t),
                P(),
                P(t, None),
                P(),
                P(s, t),
                P(s, t),
                P(t, s),
            ),
            out_specs=P(AXES, None),
            check_vma=False,
        )(*args)

    return run
```
